32 devices in a mesh: ep: 8 (over z, x), tp: 4 (over y, core).
Axes of the slice: x: 2, y: 2, z: 4, core: 2. Of those that a mesh axis runs over, the one named last changes fastest.
Arguments:
- query_latent: bfloat16 [2048, 512], P(('ep', 'tp')), may hold values from -6 to 6
- key_latent: bfloat16 [2048, 256], P(('ep', 'tp')), may hold values from -6 to 6
- rotary_key: bfloat16 [2048, 32], P(('ep', 'tp')), may hold values from -140 to 140
- query_gain: float32 [512], replicated, may hold values from 0.1 to 1.9
- latent_gain: float32 [256], replicated, may hold values from 0.1 to 1.9
- query_content: bfloat16 [512, 512], replicated, may hold values from -0.625 to 0.625
- query_rotary: bfloat16 [512, 256], replicated, may hold values from -0.625 to 0.625
- key_content: bfloat16 [256, 512], replicated, may hold values from -0.375 to 0.375
- value_weight: bfloat16 [256, 512], replicated, may hold values from -0.375 to 0.375
- output_weight: bfloat16 [512, 2048], P('tp'), may hold values from -1 to 1
- expert_input: bfloat16 [2048, 2048], P(('ep', 'tp')), may hold values from -6 to 6
- norm_gain: float32 [2048], replicated, may hold values from 0.1 to 1.9
- routes: int32 [2048, 2], P(('ep', 'tp')), may hold values from 0 to 15, all different within a row; in each aligned block of 64 rows (0 to 63, 64 to 127, ...) at most 16 rows name the same one
- route_weight: float32 [2048, 2], P(('ep', 'tp')), may hold values from 0.25 to 2
- expert_gate: bfloat16 [16, 2048, 1024], P('ep', None, 'tp'), may hold values from -0.125 to 0.125
- expert_up: bfloat16 [16, 2048, 1024], P('ep', None, 'tp'), may hold values from -0.125 to 0.125
- expert_down: bfloat16 [16, 1024, 2048], P('ep', 'tp'), may hold values from -0.1875 to 0.1875
- shared_gate: bfloat16 [2048, 1024], P(None, 'tp'), may hold values from -0.125 to 0.125
- shared_up: bfloat16 [2048, 1024], P(None, 'tp'), may hold values from -0.125 to 0.125
- shared_down: bfloat16 [1024, 2048], P('tp'), may hold values from -0.1875 to 0.1875
Outputs:
- mixer_out: bfloat16 [2048, 2048], P(('ep', 'tp'))
- expert_out: bfloat16 [2048, 2048], P(('ep', 'tp'))
The draws below stay inside these ranges and needn't reach their ends.
Inputs may be any that keep to these rules, and one draw needn't show every extreme that they name: `routes`: each row names 2 different experts. Within the rows of one device (aligned blocks of 64 rows) no expert is named by more than 16 rows, and in every draw some expert is named by exactly 16 rows of some device.
All inputs are finite; a program needn't handle non-finite values.
Results may differ from the reference program's by a relative error of at most 0.013.
The reference program's roundings to bfloat16 on the way count: a program that leaves them out, or rounds other values in their place, can miss the bound.
Values may be sent and summed in bfloat16 or wider, within the bound.
No kernel may reach another device: no remote copies, remote signals or barrier semaphores. Data moves between devices by JAX's collectives and lax.ppermute only.
A program may use at most 128 MiB of HBM per device.

```python
import math
from functools import partial
import jax
import jax.numpy as jnp
import numpy as np
from jax import lax

D = 2048
HEADS = 8
CONTENT = 64
ROTARY = 32
VALUE = 64
QUERY_RANK = 512
KEY_RANK = 256
EXPERT_WIDTH = 1024
SHARED_WIDTH = 1024
TOPK = 2
TOK_B = 64
EXPERTS = 16
CAPACITY = 16
TOKENS_A = 2048
TOKENS_B = 2048
N_EP = 8
N_TP = 4


def draw_rotary_key(key, part):
    normal_part = jnp.clip(jax.random.normal(jax.random.fold_in(key, 11), (TOKENS_A, ROTARY), jnp.float32), -6.0, 6.0)
    entries = normal_part
    return entries.astype(jnp.bfloat16)


def block_levels(rng, dims, shards, smallest, top_value):
    level = 1.0
    for dim, blocks in shards:
        draws = jax.random.uniform(jax.random.fold_in(jax.random.fold_in(rng, 6), dim), (blocks,), jnp.float32, smallest / len(shards), top_value / len(shards))
        level = level * jnp.repeat(jnp.exp(draws), dims[dim] // blocks).reshape((-1,) + (1,) * (len(dims) - 1 - dim))
    return level


def deal_out(rng, own, number, rows, amount, top, limit, slope):
    sequence = jax.random.permutation(rng, amount)
    crowded, ordinary = load_shares(amount, rows * top, limit, slope, True), load_shares(amount, rows * top, limit, slope, False)
    places = jnp.arange(amount)

    def named(sizes, turn):
        used = int((sizes > 0).sum())
        fixed = max(1, used // 4)
        moved = fixed + (places - fixed + turn * (used - fixed)) % max(1, amount - fixed)
        return jnp.zeros((amount,), jnp.int32).at[sequence[jnp.where(places < fixed, places, moved)]].set(jnp.asarray(sizes, jnp.int32))

    sizes = jnp.where(number % 4 == 0, named(crowded, number // 4), named(ordinary, number - number // 4 - 1))
    mixed = jax.random.permutation(jax.random.fold_in(own, 3), amount)
    source_of, taker = mixed[0:amount // 2 * 2:2], mixed[1:amount // 2 * 2:2]
    slack = jnp.minimum(sizes[source_of] - 1, limit - sizes[taker]) // 2
    slack = jnp.where((source_of == sequence[0]) | (taker == sequence[0]) | (sizes[taker] == 0), 0, jnp.maximum(slack, 0))
    moved = jax.random.randint(jax.random.fold_in(own, 4), (amount // 2,), 0, 1 << 20) % (slack + 1)
    sizes = sizes.at[source_of].add(-moved).at[taker].add(moved)
    labels = jnp.searchsorted(jnp.cumsum(sizes), jnp.arange(rows * top), side="right").astype(jnp.int32)
    grid = labels.reshape(top, rows).T
    grid = grid[jax.random.permutation(jax.random.fold_in(own, 1), rows)]
    turn = jax.random.randint(jax.random.fold_in(own, 2), (rows, 1), 0, top)
    return jnp.take_along_axis(grid, (jnp.arange(top)[None, :] + turn) % top, axis=1)


def load_shares(number_of, total, limit, skew, full):
    portions = [(1 << 20) // math.isqrt(rank ** skew) + 1 for rank in range(1, number_of + 1)]
    largest = limit if full else min(limit, max(-(-total // number_of), total * portions[0] // sum(portions)))
    least = 1 if total - largest >= number_of - 1 else 0
    holding, surplus = [largest] + [least] * (number_of - 1), total - largest - least * (number_of - 1)
    while surplus > 0:
        movable = [i for i in range(1, number_of) if holding[i] < largest] or [i for i in range(1, number_of) if holding[i] < limit]
        mass, budget = sum([portions[i] for i in movable]), surplus
        for i in movable:
            addition = min(limit - holding[i], max(1, budget * portions[i] // mass), surplus)
            holding[i] = holding[i] + addition
            surplus = surplus - addition
    return np.array(holding)


def gaussian(own_key, dims, scale, reach, pieces=(), held_as=jnp.bfloat16):
    values = jax.random.normal(own_key, dims, jnp.float32) * scale
    if len(pieces) > 0:
        values = block_levels(own_key, dims, pieces, -0.22, 0.18) * values
    return jnp.clip(values, min=-reach, max=reach).astype(held_as)


def setup_inputs(seed: int = 0) -> dict:
    streams_of = jax.random.split(jax.random.key(seed), 21)
    query_latent = gaussian(streams_of[0], (TOKENS_A, QUERY_RANK), 1.0, 6.0, ((0, 32),))
    key_latent = gaussian(streams_of[1], (TOKENS_A, KEY_RANK), 1.0, 6.0, ((0, 32),))
    rotary_key = draw_rotary_key(jax.random.fold_in(streams_of[20], 71), 0)
    query_gain = jnp.clip(1.0 + 0.18 * jax.random.normal(streams_of[3], (QUERY_RANK,), jnp.float32), 0.1, 1.9)
    latent_gain = jnp.clip(1.0 + 0.18 * jax.random.normal(streams_of[4], (KEY_RANK,), jnp.float32), 0.1, 1.9)
    query_content = gaussian(streams_of[5], (QUERY_RANK, HEADS * CONTENT), (QUERY_RANK // 6) ** -0.5, 0.625)
    query_rotary = gaussian(streams_of[6], (QUERY_RANK, HEADS * ROTARY), (QUERY_RANK // 6) ** -0.5, 0.625)
    key_content = gaussian(streams_of[7], (KEY_RANK, HEADS * CONTENT), KEY_RANK ** -0.5, 0.375)
    value_weight = gaussian(streams_of[8], (KEY_RANK, HEADS * VALUE), KEY_RANK ** -0.5, 0.375)
    output_weight = gaussian(streams_of[9], (HEADS * VALUE, D), (HEADS * VALUE // 16) ** -0.5, 1.0, ((0, 4),))
    expert_input = gaussian(streams_of[10], (TOKENS_B, D), 1.0, 6.0, ((0, 32),))
    norm_gain = jnp.clip(1.0 + 0.18 * jax.random.normal(streams_of[11], (D,), jnp.float32), 0.1, 1.9)
    routes_keys = jax.random.split(jax.random.fold_in(streams_of[12], 1), TOKENS_B // TOK_B)
    routes_turns = jax.random.permutation(jax.random.fold_in(streams_of[12], 3), TOKENS_B // TOK_B)
    routes = jax.vmap(lambda own, number: deal_out(jax.random.fold_in(streams_of[12], 2), own, number, TOK_B, EXPERTS, TOPK, CAPACITY, 1))(routes_keys, routes_turns).reshape((TOKENS_B, TOPK))
    route_weight = jnp.clip(0.25 + 1.75 * jax.random.uniform(streams_of[13], (TOKENS_B, TOPK), jnp.float32) ** block_levels(streams_of[13], (TOKENS_B, TOPK), ((0, 32),), -0.2, 0.2), 0.25, 2.0)
    expert_gate = gaussian(streams_of[14], (EXPERTS, D, EXPERT_WIDTH), D ** -0.5, 0.125, ((0, 8), (2, 4)))
    expert_up = gaussian(streams_of[15], (EXPERTS, D, EXPERT_WIDTH), D ** -0.5, 0.125, ((0, 8), (2, 4)))
    expert_down = gaussian(streams_of[16], (EXPERTS, EXPERT_WIDTH, D), EXPERT_WIDTH ** -0.5, 0.1875, ((0, 8), (1, 4)))
    shared_gate = gaussian(streams_of[17], (D, SHARED_WIDTH), D ** -0.5, 0.125, ((1, 4),))
    shared_up = gaussian(streams_of[18], (D, SHARED_WIDTH), D ** -0.5, 0.125, ((1, 4),))
    shared_down = gaussian(streams_of[19], (SHARED_WIDTH, D), SHARED_WIDTH ** -0.5, 0.1875, ((0, 4),))
    return {"query_latent": query_latent, "key_latent": key_latent, "rotary_key": rotary_key, "query_gain": query_gain, "latent_gain": latent_gain, "query_content": query_content, "query_rotary": query_rotary, "key_content": key_content, "value_weight": value_weight, "output_weight": output_weight, "expert_input": expert_input, "norm_gain": norm_gain, "routes": routes, "route_weight": route_weight, "expert_gate": expert_gate, "expert_up": expert_up, "expert_down": expert_down, "shared_gate": shared_gate, "shared_up": shared_up, "shared_down": shared_down}


norm_eps = 1e-06
rope_base = 10000.0

def rms_rows(entries, gain_row):
    widened = entries.astype(jnp.float32)
    return widened * lax.rsqrt(lax.optimization_barrier(jnp.mean(widened * widened, -1, keepdims=True)) + norm_eps) * gain_row.astype(jnp.float32)

def turn_pairs(entries, positions):
    width_full = entries.shape[-1]
    frequency = rope_base ** (-jnp.arange(width_full // 2, dtype=jnp.float32) * 2.0 / width_full)
    angles = positions.astype(jnp.float32)[:, None] * frequency[None, :]
    cosine = jnp.cos(angles)[:, None, :]
    sine_part = jnp.sin(angles)[:, None, :]
    even_part = entries[..., 0::2]
    odd_part = entries[..., 1::2]
    joined = jnp.stack([even_part * cosine - odd_part * sine_part, even_part * sine_part + odd_part * cosine], -1)
    return joined.reshape(entries.shape)

def feed_forward(row_block, gate_weight, up_weight, down_weight, groups):
    gated = jnp.dot(row_block, gate_weight, preferred_element_type=jnp.float32)
    lifted = jnp.dot(row_block, up_weight, preferred_element_type=jnp.float32)
    hidden = (jax.nn.silu(gated) * lifted).astype(jnp.bfloat16)
    group_width = hidden.shape[1] // groups
    running = jnp.zeros((row_block.shape[0], down_weight.shape[1]), jnp.float32)
    for group_index in range(groups):
        product = jnp.dot(hidden[:, group_index * group_width:(group_index + 1) * group_width], down_weight[group_index * group_width:(group_index + 1) * group_width], preferred_element_type=jnp.float32)
        running = running + lax.optimization_barrier(product.astype(jnp.bfloat16)).astype(jnp.float32)
    return running

def attend_queries(query_blocks, key_wide, turn_wide, value_wide):
    query_part, query_turn = query_blocks
    score_scale = (CONTENT + ROTARY) ** (-0.5)
    scores = jnp.einsum('qhc,khc->qhk', query_part.astype(jnp.float32), key_wide)
    scores = scores + jnp.einsum('qhr,kr->qhk', query_turn.astype(jnp.float32), turn_wide)
    scores = scores * score_scale
    weights = jnp.exp(scores - lax.optimization_barrier(jnp.max(scores, -1, keepdims=True)))
    denominator = lax.optimization_barrier(jnp.sum(weights, -1))
    rounded = lax.optimization_barrier(weights.astype(jnp.bfloat16)).astype(jnp.float32)
    numerator = jnp.einsum('qhk,khv->qhv', rounded, value_wide)
    return (numerator / denominator[..., None]).astype(jnp.bfloat16)

def block_slots(route_block):
    flat_routes = route_block.reshape(-1)
    marks = (flat_routes[:, None] == jnp.arange(EXPERTS, dtype=jnp.int32)[None, :]).astype(jnp.int32)
    return lax.optimization_barrier(jnp.sum((jnp.cumsum(marks, 0) - marks) * marks, 1)).reshape(route_block.shape)

def reference(query_latent, key_latent, rotary_key, query_gain, latent_gain, query_content, query_rotary, key_content, value_weight, output_weight, expert_input, norm_gain, routes, route_weight, expert_gate, expert_up, expert_down, shared_gate, shared_up, shared_down):
    row_count = query_latent.shape[0]
    positions = jnp.arange(row_count, dtype=jnp.int32)
    query_normed = rms_rows(query_latent, query_gain).astype(jnp.bfloat16)
    latent_normed = rms_rows(key_latent, latent_gain).astype(jnp.bfloat16)
    query_part = jnp.dot(query_normed, query_content, preferred_element_type=jnp.float32).astype(jnp.bfloat16).reshape(row_count, HEADS, CONTENT)
    query_turn = turn_pairs(jnp.dot(query_normed, query_rotary, preferred_element_type=jnp.float32).reshape(row_count, HEADS, ROTARY), positions).astype(jnp.bfloat16)
    key_turn = turn_pairs(rotary_key.astype(jnp.float32)[:, None, :], positions)[:, 0, :].astype(jnp.bfloat16)
    key_part = jnp.dot(latent_normed, key_content, preferred_element_type=jnp.float32).astype(jnp.bfloat16).reshape(row_count, HEADS, CONTENT)
    value_rows = jnp.dot(latent_normed, value_weight, preferred_element_type=jnp.float32).astype(jnp.bfloat16).reshape(row_count, HEADS, VALUE)
    query_block = math.gcd(row_count, 256)
    block_count = row_count // query_block
    query_blocks = (query_part.reshape(block_count, query_block, HEADS, CONTENT), query_turn.reshape(block_count, query_block, HEADS, ROTARY))
    attended = lax.map(partial(attend_queries, key_wide=key_part.astype(jnp.float32), turn_wide=key_turn.astype(jnp.float32), value_wide=value_rows.astype(jnp.float32)), query_blocks)
    attended = attended.reshape(row_count, HEADS * VALUE)
    group_width = HEADS * VALUE // N_TP
    mixed = jnp.zeros((row_count, output_weight.shape[1]), jnp.float32)
    for group_index in range(N_TP):
        product = jnp.dot(attended[:, group_index * group_width:(group_index + 1) * group_width], output_weight[group_index * group_width:(group_index + 1) * group_width], preferred_element_type=jnp.float32)
        mixed = mixed + lax.optimization_barrier(product.astype(jnp.bfloat16)).astype(jnp.float32)
    mixer_out = mixed.astype(jnp.bfloat16)
    token_count = expert_input.shape[0]
    device_count = N_EP * N_TP
    per_device = token_count // device_count
    expert_normed = rms_rows(expert_input, norm_gain).astype(jnp.bfloat16)
    slots = jax.vmap(block_slots)(routes.reshape(device_count, per_device, TOPK)).reshape(token_count, TOPK)
    device_of = (jnp.arange(token_count, dtype=jnp.int32) // per_device).astype(jnp.int32)
    token_index = jnp.broadcast_to(jnp.arange(token_count, dtype=jnp.int32)[:, None], (token_count, TOPK))
    table = jnp.full((EXPERTS, device_count, CAPACITY), token_count, jnp.int32)
    table = table.at[routes, jnp.broadcast_to(device_of[:, None], (token_count, TOPK)), slots].set(token_index)
    padded = jnp.concatenate([expert_normed, jnp.zeros((1, expert_normed.shape[1]), jnp.bfloat16)], 0)

    def one_expert(expert_args):
        table_row, gate_weight, up_weight, down_weight = expert_args
        row_block = padded[table_row.reshape(-1)]
        return feed_forward(row_block, gate_weight, up_weight, down_weight, N_TP).astype(jnp.bfloat16)
    results = lax.map(one_expert, (table, expert_gate, expert_up, expert_down))
    flat_index = (routes * (device_count * CAPACITY) + device_of[:, None] * CAPACITY + slots).astype(jnp.int32)
    picked = results.reshape(-1, results.shape[-1])[flat_index.reshape(-1)].reshape(token_count, TOPK, -1)
    routed = lax.optimization_barrier(jnp.sum(route_weight.astype(jnp.float32)[..., None] * picked.astype(jnp.float32), 1))
    shared_sum = feed_forward(expert_normed, shared_gate, shared_up, shared_down, N_TP)
    expert_out = (routed + shared_sum).astype(jnp.bfloat16)
    return (mixer_out, expert_out)
```

```python
import functools

import jax
import jax.numpy as jnp
from jax import lax
from jax.experimental import pallas as pl
from jax.sharding import PartitionSpec as P


HEADS = 8
CONTENT = 64
ROTARY = 32
VALUE = 64
CHUNKS = 2

norm_eps = 1e-06
rope_base = 10000.0


def rms_rows(entries, gain_row):
    widened = entries.astype(jnp.float32)
    return widened * lax.rsqrt(jnp.mean(widened * widened, -1, keepdims=True) + norm_eps) * gain_row


def dot32(left, right):
    return jnp.dot(left, right, preferred_element_type=jnp.float32)


def turn_tables(positions, width, period):
    column = lax.broadcasted_iota(jnp.int32, (1, width), 1)
    pair = ((column % period) // 2).astype(jnp.float32)
    frequency = rope_base ** (-pair * 2.0 / period)
    angles = positions.astype(jnp.float32)[:, None] * frequency
    return jnp.cos(angles), jnp.sin(angles)


def swap_matrix(width):
    row = lax.broadcasted_iota(jnp.int32, (width, width), 0)
    column = lax.broadcasted_iota(jnp.int32, (width, width), 1)
    partner = row == (column ^ 1)
    sign = jnp.where(column % 2 == 0, -1.0, 1.0)
    return jnp.where(partner, sign, 0.0).astype(jnp.bfloat16)


def swap_tp(entries, distance):
    size = lax.axis_size("tp")
    return lax.ppermute(entries, "tp", [(i, i ^ distance) for i in range(size)])


def gather_far(entries):
    return [swap_tp(entries, k) for k in range(2, lax.axis_size("tp"), 2)]


def gather_near(entries, far):
    pieces = []
    for piece in [entries] + far:
        pieces.append(piece)
        if lax.axis_size("tp") > 1:
            pieces.append(swap_tp(piece, 1))
    return pieces


def swap_ep(entries, distance):
    size = lax.axis_size("ep")
    return lax.ppermute(entries, "ep", [(i, i ^ distance) for i in range(size)])


def exchange_fits(size):
    return 2 <= size <= 16 and size & (size - 1) == 0


def merge_pairs(parts):
    size = parts.shape[0]
    if size == 1:
        return (parts[0].astype(jnp.float32),)
    received = swap_tp(parts[1::2], 1)
    merged = parts[0::2].astype(jnp.float32) + received.astype(jnp.float32)
    return (merged[0],) + tuple(merged[k].astype(jnp.bfloat16) for k in range(1, size // 2))


def send_pairs(merged):
    return [swap_tp(merged[k], 2 * k) for k in range(1, len(merged))]


def sum_pairs(merged, arrived):
    total = merged[0]
    for piece in arrived:
        total = total + piece.astype(jnp.float32)
    return total


def attend_kernel(query_ref, turn_ref, latent_ref, key_ref, value_ref, out_ref):
    own = query_ref.shape[1]
    wide = query_ref.shape[2]
    heads = wide // CONTENT
    rank = key_ref.shape[0]
    latent = latent_ref[:, :rank]
    keys = dot32(latent, key_ref[...]).astype(jnp.bfloat16)
    values = dot32(latent, value_ref[...]).astype(jnp.bfloat16)
    query = query_ref[0]
    head_of = lax.broadcasted_iota(jnp.int32, (own, wide), 1) // CONTENT
    stacked = jnp.concatenate(
        [jnp.where(head_of == h, query, jnp.zeros_like(query)) for h in range(heads)], 0
    )
    contract = (((1,), (1,)), ((), ()))
    scores = lax.dot_general(stacked, keys, contract, preferred_element_type=jnp.float32)
    scores = scores + lax.dot_general(
        turn_ref[0], latent_ref[:, rank:], contract, preferred_element_type=jnp.float32
    )
    scores = scores * ((CONTENT + ROTARY) ** (-0.5))
    weights = jnp.exp(scores - jnp.max(scores, -1, keepdims=True))
    total = jnp.sum(weights, -1, keepdims=True)
    result = dot32(weights.astype(jnp.bfloat16), values) / total
    joined = result[:own]
    for h in range(1, heads):
        joined = jnp.where(head_of == h, result[h * own : (h + 1) * own], joined)
    out_ref[0] = joined.astype(jnp.bfloat16)


def attend(query, turned, all_keys, key_content, value_weight):
    groups, own, wide = query.shape
    count = all_keys.shape[0]
    rank = key_content.shape[0]
    return pl.pallas_call(
        attend_kernel,
        grid=(groups,),
        in_specs=[
            pl.BlockSpec((1, own, wide), lambda g: (g, 0, 0)),
            pl.BlockSpec((1,) + turned.shape[1:], lambda g: (g, 0, 0)),
            pl.BlockSpec(all_keys.shape, lambda g: (0, 0)),
            pl.BlockSpec((rank, wide), lambda g: (0, g)),
            pl.BlockSpec((rank, wide), lambda g: (0, g)),
        ],
        out_specs=pl.BlockSpec((1, own, wide), lambda g: (g, 0, 0)),
        out_shape=jax.ShapeDtypeStruct((groups, own, wide), jnp.bfloat16),
        cost_estimate=pl.CostEstimate(
            flops=4 * groups * count * wide * (rank + own * 2),
            transcendentals=groups * own * count * 2,
            bytes_accessed=4 * count * rank,
        ),
        name="attend",
    )(query, turned, all_keys, key_content, value_weight)


def attend_chunked(query, turned, all_keys, key_content, value_weight):
    groups, own, wide = query.shape
    heads = wide // CONTENT
    count = all_keys.shape[0]
    rank = key_content.shape[0]
    latent, key_turn = all_keys[:, :rank], all_keys[:, rank:]
    block = min(count, 2048)
    query = query.reshape(groups, own, heads, CONTENT)
    turned = turned.reshape(groups, heads, own, ROTARY)

    def advance(state, pieces):
        peak, total, summed = state
        latent_rows, turn_rows = pieces
        keys = dot32(latent_rows, key_content).astype(jnp.bfloat16)
        values = dot32(latent_rows, value_weight).astype(jnp.bfloat16)
        keys = keys.reshape(block, groups, heads, CONTENT)
        values = values.reshape(block, groups, heads, VALUE)
        scores = jnp.einsum("gqhc,kghc->ghqk", query, keys, preferred_element_type=jnp.float32)
        scores = scores + jnp.einsum(
            "ghqr,kr->ghqk", turned, turn_rows, preferred_element_type=jnp.float32
        )
        scores = scores * ((CONTENT + ROTARY) ** (-0.5))
        fresh = jnp.maximum(peak, jnp.max(scores, -1))
        factor = jnp.exp(peak - fresh)
        weights = jnp.exp(scores - fresh[..., None])
        total = total * factor + jnp.sum(weights, -1)
        summed = summed * factor[..., None] + jnp.einsum(
            "ghqk,kghv->ghqv",
            weights.astype(jnp.bfloat16),
            values,
            preferred_element_type=jnp.float32,
        )
        return (fresh, total, summed), None

    start = (
        jnp.full((groups, heads, own), -jnp.inf, jnp.float32),
        jnp.zeros((groups, heads, own), jnp.float32),
        jnp.zeros((groups, heads, own, VALUE), jnp.float32),
    )
    stacked = (
        latent.reshape(count // block, block, latent.shape[1]),
        key_turn.reshape(count // block, block, key_turn.shape[1]),
    )
    (peak, total, summed), _ = lax.scan(advance, start, stacked)
    result = (summed / total[..., None]).astype(jnp.bfloat16)
    return result.transpose(0, 2, 1, 3).reshape(groups, own, wide)


def feed_forward(row_block, gate_weight, up_weight, down_weight):
    gated = dot32(row_block, gate_weight)
    lifted = dot32(row_block, up_weight)
    hidden = (jax.nn.silu(gated) * lifted).astype(jnp.bfloat16)
    return dot32(hidden, down_weight).astype(jnp.bfloat16)


def shards(
    query_latent,
    key_latent,
    rotary_key,
    query_gain,
    latent_gain,
    query_content,
    query_rotary,
    key_content,
    value_weight,
    output_weight,
    expert_input,
    norm_gain,
    routes,
    route_weight,
    expert_gate,
    expert_up,
    expert_down,
    shared_gate,
    shared_up,
    shared_down,
):
    tp_size = lax.axis_size("tp")
    ep_size = lax.axis_size("ep")
    tp_index = lax.axis_index("tp")
    own_rows = query_latent.shape[0]
    own_start = (lax.axis_index("ep") * tp_size + tp_index) * own_rows
    positions = own_start + jnp.arange(own_rows, dtype=jnp.int32)
    token_rows, model_width = expert_input.shape
    picks = routes.shape[1]
    local_experts = expert_gate.shape[0]
    expert_total = local_experts * ep_size
    capacity = 2 * token_rows * picks // expert_total
    slot_total = expert_total * capacity

    expert_normed = rms_rows(expert_input, norm_gain).astype(jnp.bfloat16)
    flat_routes = routes.reshape(-1)
    marks = (flat_routes[:, None] == jnp.arange(expert_total, dtype=jnp.int32)[None, :]).astype(
        jnp.bfloat16
    )
    pick_count = token_rows * picks
    before = (
        lax.broadcasted_iota(jnp.int32, (pick_count, pick_count), 1)
        < lax.broadcasted_iota(jnp.int32, (pick_count, pick_count), 0)
    ).astype(jnp.bfloat16)
    ranks = jnp.sum(dot32(before, marks) * marks.astype(jnp.float32), 1).astype(jnp.int32)
    targets = (
        (flat_routes % local_experts) * ep_size + flat_routes // local_experts
    ) * capacity + ranks
    targets = targets.reshape(token_rows, picks)
    slots = jnp.arange(slot_total, dtype=jnp.int32)
    chosen = [
        (targets[:, k : k + 1] == slots[None, :]).astype(jnp.bfloat16) for k in range(picks)
    ]
    picker = functools.reduce(jnp.add, chosen)
    chunks = CHUNKS if local_experts % CHUNKS == 0 else 1
    chunk_experts = local_experts // chunks
    chunk_slots = slot_total // chunks
    outgoing = (
        lax.dot_general(
            picker, expert_normed, (((0,), (0,)), ((), ())), preferred_element_type=jnp.float32
        )
        .astype(jnp.bfloat16)
        .reshape(local_experts, ep_size, capacity, model_width)
    )
    latent_normed = rms_rows(key_latent, latent_gain).astype(jnp.bfloat16)
    cosine, sine = turn_tables(positions, ROTARY, ROTARY)
    key_turned = (
        rotary_key.astype(jnp.float32) * cosine + dot32(rotary_key, swap_matrix(ROTARY)) * sine
    ).astype(jnp.bfloat16)
    column_keys = jnp.concatenate([latent_normed, key_turned], 1)
    if exchange_fits(ep_size):
        column_keys = jnp.concatenate([column_keys, swap_ep(column_keys, 1)], 0)
    outgoing, column_keys, query_latent = lax.optimization_barrier(
        (outgoing, column_keys, query_latent)
    )
    if exchange_fits(ep_size):
        pieces = [swap_ep(column_keys, k) for k in range(2, ep_size, 2)]
        column_keys = jnp.concatenate([column_keys] + pieces, 0)
    else:
        column_keys = lax.all_gather(column_keys, "ep", axis=0, tiled=True)
    received = lax.all_to_all(outgoing, "ep", split_axis=1, concat_axis=1, tiled=True)
    weight_far = gather_far(output_weight)
    received = received.reshape(local_experts, ep_size * capacity, model_width)
    all_keys = jnp.concatenate(gather_near(column_keys, gather_far(column_keys)), 0)
    token_pieces = gather_near(expert_normed, gather_far(expert_normed))
    weight_pieces = gather_near(output_weight, weight_far)

    query_normed = rms_rows(query_latent, query_gain).astype(jnp.bfloat16)
    query_part = dot32(query_normed, query_content).astype(jnp.bfloat16)
    turn_width = query_rotary.shape[1]
    cosine, sine = turn_tables(positions, turn_width, ROTARY)
    swapped_rotary = dot32(query_rotary, swap_matrix(turn_width)).astype(jnp.bfloat16)
    query_turn = (
        dot32(query_normed, query_rotary) * cosine + dot32(query_normed, swapped_rotary) * sine
    ).astype(jnp.bfloat16)
    group_heads = HEADS // tp_size
    query_groups = query_part.reshape(own_rows, tp_size, group_heads * CONTENT).transpose(1, 0, 2)
    turn_groups = (
        query_turn.reshape(own_rows, tp_size, group_heads, ROTARY)
        .transpose(1, 2, 0, 3)
        .reshape(tp_size, group_heads * own_rows, ROTARY)
    )
    mix = attend if all_keys.shape[0] <= 4096 else attend_chunked
    attended = mix(
        query_groups,
        turn_groups,
        all_keys,
        key_content,
        value_weight,
    )
    received, attended, token_pieces, weight_pieces = lax.optimization_barrier(
        (received, attended, token_pieces, weight_pieces)
    )
    mixed = None
    for k, piece in enumerate(weight_pieces):
        columns = lax.dynamic_index_in_dim(attended, tp_index ^ k, 0, keepdims=False)
        product = dot32(columns, piece).astype(jnp.bfloat16).astype(jnp.float32)
        mixed = product if mixed is None else mixed + product
    mixer_out = mixed.astype(jnp.bfloat16)

    shared_term = feed_forward(
        jnp.concatenate(token_pieces, 0), shared_gate, shared_up, shared_down
    ).reshape(tp_size, token_rows, model_width)

    returned = []
    routed = [received[c * chunk_experts : (c + 1) * chunk_experts] for c in range(chunks)]
    far = gather_far(routed[0])
    far, shared_term, routed = lax.optimization_barrier((far, shared_term, routed))
    shared_merged = merge_pairs(shared_term)
    for c in range(chunks):
        pieces = gather_near(routed[c], far)
        if c + 1 < chunks:
            far = gather_far(routed[c + 1])
        terms = []
        for x in range(chunk_experts):
            e = c * chunk_experts + x
            rows = jnp.concatenate([piece[x] for piece in pieces], 0)
            term = feed_forward(rows, expert_gate[e], expert_up[e], expert_down[e])
            terms.append(term.reshape(tp_size, 1, ep_size * capacity, model_width))
        parts = terms[0] if chunk_experts == 1 else jnp.concatenate(terms, 1)
        merged = merge_pairs(parts)
        if c == chunks - 1:
            merged, shared_merged = lax.optimization_barrier((merged, shared_merged))
        arrived = send_pairs(merged)
        returned.append(sum_pairs(merged, arrived))
    shared_sum = sum_pairs(shared_merged, send_pairs(shared_merged))
    for c in range(chunks):
        summed = returned[c].astype(jnp.bfloat16)
        summed = summed.reshape(chunk_experts, ep_size, capacity, model_width)
        summed = lax.all_to_all(summed, "ep", split_axis=1, concat_axis=1, tiled=True)
        returned[c] = summed.reshape(chunk_slots, model_width)
    combined = shared_sum
    for k in range(picks):
        picked = None
        for c in range(chunks):
            piece = dot32(chosen[k][:, c * chunk_slots : (c + 1) * chunk_slots], returned[c])
            picked = piece if picked is None else picked + piece
        combined = combined + route_weight[:, k : k + 1] * picked
    expert_out = combined.astype(jnp.bfloat16)
    return (mixer_out, expert_out)


def solution(mesh):
    rows = P(("ep", "tp"), None)
    in_specs = (
        rows,
        rows,
        rows,
        P(),
        P(),
        P(),
        P(),
        P(),
        P(),
        P("tp", None),
        rows,
        P(),
        rows,
        rows,
        P("ep", None, "tp"),
        P("ep", None, "tp"),
        P("ep", "tp", None),
        P(None, "tp"),
        P(None, "tp"),
        P("tp", None),
    )

    return jax.shard_map(
        shards, mesh=mesh, in_specs=in_specs, out_specs=(rows, rows), check_vma=False
    )
```
